32 devices in a mesh: grp: 2 (over y), sp: 4 (over z), tp: 4 (over x, core).
Axes of the slice: x: 2, y: 2, z: 4, core: 2. Of those that a mesh axis runs over, the one named last changes fastest.
Arguments:
- residual: bfloat16 [2048, 2048], P(('grp', 'sp')), parts along dimension 0, may hold values from -6 to 6
- queries: bfloat16 [2048, 1024], P(('grp', 'sp'), 'tp'), parts along dimension 0, may hold values from -400 to 400
- keys: bfloat16 [2048, 1024], P(('grp', 'sp'), 'tp'), parts along dimension 0, may hold values from -8 to 8
- values: bfloat16 [2048, 1024], P(('grp', 'sp'), 'tp'), parts along dimension 0, may hold values from -6 to 6
- log_gates: float32 [2048, 16], P(('grp', 'sp'), 'tp'), parts along dimension 0, may hold values from -126 to 0, as said below
- w_out: bfloat16 [1024, 2048], P('tp'), may hold values from -0.75 to 0.75
- norm_gain: float32 [2048], replicated, may hold values from 0.1 to 1.9
- w_gate: bfloat16 [2048, 5632], P('sp', 'tp'), may hold values from -0.125 to 0.125
- w_up: bfloat16 [2048, 5632], P('sp', 'tp'), may hold values from -0.125 to 0.125
- w_down: bfloat16 [5632, 2048], P('tp', 'sp'), may hold values from -0.078125 to 0.078125
Outputs:
- output: bfloat16 [2048, 2048], P(('grp', 'sp', 'tp')), parts along dimension 0
The draws below stay inside these ranges and needn't reach their ends.
There are 2 independent parts, one for each index of `grp`. The reference program is written for one: setup_inputs(seed, part) draws one part's arguments, and reference() takes and returns one part's arrays. A program takes and returns all parts, laid end to end along the dimension named above; an argument that names none is the same for every part. Nothing has to cross between parts.
Inputs may be any that keep to these rules, and one draw needn't show every extreme that they name: `log_gates`: never rises along positions.
All inputs are finite; a program needn't handle non-finite values.
Results may differ from the reference program's by a relative error of at most 0.014.
Values may be sent and summed in bfloat16 or wider, within the bound.
A program may use at most 128 MiB of HBM per device.

```python
import math
import jax
import jax.numpy as jnp
from jax import lax

D = 2048
ATTN_HEAD_COUNT = 16
HEAD_DIM = 64
FF = 5632
TOK_DEV = 256
SEQUENCE_TOKENS = 1024
N_TP = 4


def layout(key):
    random_seed_key = jax.random.fold_in(key, 31)
    random_ordering_key, random_shift_key, random_back_key, random_stride_key, random_spacing_key, random_strong_key, random_select_key, random_spike_key = jax.random.split(random_seed_key, 8)
    block_count = SEQUENCE_TOKENS // TOK_DEV
    inserted_count = block_count - 2
    quarter = max(TOK_DEV // 4, 1)
    head_order = jax.random.permutation(random_ordering_key, ATTN_HEAD_COUNT)
    gradual_heads = head_order < ATTN_HEAD_COUNT // 2
    block_ids = jnp.arange(inserted_count, dtype=jnp.int32) + 2
    places = block_ids * TOK_DEV + jax.random.randint(random_shift_key, (inserted_count,), 0, quarter)
    matches = (block_ids - 1) * TOK_DEV - 1 - jax.random.randint(random_back_key, (inserted_count,), 0, quarter)
    neighbours = matches - jax.random.randint(random_stride_key, (inserted_count,), 1, 5)
    score_gaps = jax.random.uniform(random_spacing_key, (inserted_count, ATTN_HEAD_COUNT), jnp.float32, 1.0, 2.5)
    strong_decline = jax.random.uniform(random_strong_key, (inserted_count, ATTN_HEAD_COUNT), jnp.float32, math.log(0.02), math.log(0.1))
    picked = jax.random.permutation(random_select_key, inserted_count)[:2]
    sudden_spike = jnp.any(jnp.arange(inserted_count, dtype=jnp.int32)[:, None] == picked[None, :], axis=1)
    sudden_decline = jax.random.uniform(random_spike_key, (inserted_count, ATTN_HEAD_COUNT), jnp.float32, math.log(0.5), math.log(0.8))
    gate_changes = jnp.where(gradual_heads[None, :], jnp.where(sudden_spike[:, None], sudden_decline, 0.0), strong_decline)
    return (gradual_heads, places, matches, neighbours, score_gaps, gate_changes)


def planted(key):
    gradual_heads, places, matches, neighbours, score_gaps, gate_changes = layout(key)
    key_query, key_keys = jax.random.split(jax.random.fold_in(key, 11), 2)
    row_width = ATTN_HEAD_COUNT * HEAD_DIM
    query_rows = jnp.clip(jax.random.normal(key_query, (SEQUENCE_TOKENS, row_width), jnp.float32), -6.0, 6.0)
    key_rows = jnp.clip(jax.random.normal(key_keys, (SEQUENCE_TOKENS, row_width), jnp.float32), -6.0, 6.0)
    inserted_count = places.shape[0]
    levels = jnp.array([8.0, 12.0, 16.0], jnp.float32)
    strength = levels[jnp.arange(inserted_count, dtype=jnp.int32) % 3][:, None, None]
    chosen = key_rows[matches].reshape(inserted_count, ATTN_HEAD_COUNT, HEAD_DIM)
    energy = jnp.maximum(jnp.sum(chosen * chosen, axis=-1, keepdims=True), 0.5 * HEAD_DIM)
    planted_rows = strength * 8.0 * math.sqrt(HEAD_DIM) * chosen / energy
    compensate = (score_gaps + gate_changes)[:, :, None]
    neighbour = chosen * (1.0 - compensate / (8.0 * strength))
    query_rows = jnp.clip(query_rows.at[places].set(planted_rows.reshape(inserted_count, row_width)), -400.0, 400.0)
    key_rows = key_rows.at[neighbours].set(neighbour.reshape(inserted_count, row_width))
    return (query_rows, key_rows)


def draw_queries(key, part):
    return planted(key)[0].astype(jnp.bfloat16)


def draw_keys(key, part):
    return planted(key)[1].astype(jnp.bfloat16)


def draw_log_gates(key, part):
    gradual_heads, places, matches, neighbours, score_gaps, gate_changes = layout(key)
    key_factor, key_jitter = jax.random.split(jax.random.fold_in(key, 23), 2)
    block_count = SEQUENCE_TOKENS // TOK_DEV
    block_factor = jnp.exp(jax.random.uniform(key_factor, (block_count, ATTN_HEAD_COUNT), jnp.float32, math.log(0.5), math.log(2.0)))
    block_factor = jnp.repeat(block_factor, TOK_DEV, axis=0)
    roughness = jax.random.uniform(key_jitter, (SEQUENCE_TOKENS, ATTN_HEAD_COUNT), jnp.float32, 0.5, 1.5)
    head_rates = jnp.where(gradual_heads, 0.5 / SEQUENCE_TOKENS, 1.0 / 40.0)
    forget_logits = -head_rates[None, :] * block_factor * roughness
    clusters = jnp.zeros((SEQUENCE_TOKENS, ATTN_HEAD_COUNT), jnp.float32).at[matches].set(gate_changes)
    return jnp.cumsum(forget_logits + clusters, axis=0)


def shard_levels(key, dims, cuts, least, largest):
    def one(position, shards_of):
        steps = jax.random.uniform(jax.random.fold_in(jax.random.fold_in(key, 6), position), (shards_of,), jnp.float32, least / len(cuts), largest / len(cuts))
        return jnp.repeat(jnp.exp(steps), dims[position] // shards_of).reshape((-1,) + (1,) * (len(dims) - position - 1))

    level = one(*cuts[0])
    for cut in cuts[1:]:
        level = level * one(*cut)
    return level


def gaussian(key, shape, spread, limit, shards=(), kind=jnp.bfloat16):
    loudness = shard_levels(key, shape, shards, -0.22, 0.18) if shards else 1.0
    entries = jax.random.normal(key, shape, jnp.float32) * spread * loudness
    return jnp.minimum(jnp.maximum(entries, -limit), limit).astype(kind)


def setup_inputs(seed: int = 0, part: int = 0) -> dict:
    seeds = jax.random.split(jax.random.key(seed), 11)
    part_splits = jax.random.split(jax.random.fold_in(seeds[10], part), 11)
    return {
        "residual": gaussian(part_splits[0], (SEQUENCE_TOKENS, D), 1.0, 6.0, ((0, 4),)),
        "queries": draw_queries(jax.random.fold_in(jax.random.fold_in(seeds[10], part), 71), part),
        "keys": draw_keys(jax.random.fold_in(jax.random.fold_in(seeds[10], part), 71), part),
        "values": gaussian(part_splits[3], (SEQUENCE_TOKENS, ATTN_HEAD_COUNT * HEAD_DIM), 1.0, 6.0, ((0, 4), (1, 4))),
        "log_gates": draw_log_gates(jax.random.fold_in(jax.random.fold_in(seeds[10], part), 71), part),
        "w_out": gaussian(seeds[5], (ATTN_HEAD_COUNT * HEAD_DIM, D), HEAD_DIM ** -0.5, 0.75, ((0, 4),)),
        "norm_gain": jnp.clip(1.0 + 0.18 * jax.random.normal(seeds[6], (D,), jnp.float32), 0.1, 1.9),
        "w_gate": gaussian(seeds[7], (D, FF), D ** -0.5, 0.125, ((0, 4), (1, 4))),
        "w_up": gaussian(seeds[8], (D, FF), D ** -0.5, 0.125, ((0, 4), (1, 4))),
        "w_down": gaussian(seeds[9], (FF, D), FF ** -0.5, 0.078125, ((0, 4), (1, 4))),
    }


def normalize(rows_in, gain):
    floats = rows_in.astype(jnp.float32)
    scaled = floats * lax.rsqrt(lax.optimization_barrier(jnp.mean(floats * floats, axis=-1, keepdims=True)) + 1e-06)
    return (scaled * gain).astype(jnp.bfloat16)

def group_sum(left, right, groups):
    rows_total = left.shape[0]
    width = left.shape[1] // groups
    left_groups = left.reshape(rows_total, groups, width).astype(jnp.float32)
    right_groups = right.reshape(groups, width, right.shape[1]).astype(jnp.float32)
    partial_terms = jnp.einsum('tgc,gcd->gtd', left_groups, right_groups).astype(jnp.bfloat16)
    partial_terms = lax.optimization_barrier(partial_terms)
    return lax.optimization_barrier(jnp.sum(partial_terms.astype(jnp.float32), axis=0))

def reference(residual, queries, keys, values, log_gates, w_out, norm_gain, w_gate, w_up, w_down):
    score_scale = HEAD_DIM ** (-0.5)
    query_heads = queries.reshape(SEQUENCE_TOKENS, ATTN_HEAD_COUNT, HEAD_DIM)
    key_heads = keys.reshape(SEQUENCE_TOKENS, ATTN_HEAD_COUNT, HEAD_DIM).astype(jnp.float32)
    value_heads = values.reshape(SEQUENCE_TOKENS, ATTN_HEAD_COUNT, HEAD_DIM).astype(jnp.float32)
    block_rows = math.gcd(SEQUENCE_TOKENS, 512)
    key_positions = jnp.arange(SEQUENCE_TOKENS, dtype=jnp.int32)

    def one_block(index_block):
        anchor = (index_block * block_rows).astype(jnp.int32)
        query_block = lax.dynamic_slice_in_dim(query_heads, anchor, block_rows, 0).astype(jnp.float32)
        gate_block = lax.dynamic_slice_in_dim(log_gates, anchor, block_rows, 0)
        scores = jnp.einsum('qhd,khd->hqk', query_block, key_heads) * score_scale
        scores = scores + gate_block.T[:, :, None] - log_gates.T[:, None, :]
        query_positions = anchor + jnp.arange(block_rows, dtype=jnp.int32)
        causal = query_positions[:, None] >= key_positions[None, :]
        scores = jnp.where(causal[None], scores, -jnp.inf)
        row_max = lax.optimization_barrier(jnp.max(scores, axis=-1, keepdims=True))
        weights = jnp.where(causal[None], jnp.exp(scores - row_max), 0.0)
        totals = lax.optimization_barrier(jnp.sum(weights, axis=-1))
        rounded = lax.optimization_barrier(weights.astype(jnp.bfloat16)).astype(jnp.float32)
        summed = jnp.einsum('hqk,khd->hqd', rounded, value_heads) / totals[:, :, None]
        return summed.transpose(1, 0, 2).reshape(block_rows, ATTN_HEAD_COUNT * HEAD_DIM).astype(jnp.bfloat16)
    attended = lax.map(one_block, jnp.arange(SEQUENCE_TOKENS // block_rows, dtype=jnp.int32))
    attended = attended.reshape(SEQUENCE_TOKENS, ATTN_HEAD_COUNT * HEAD_DIM)
    projected = group_sum(attended, w_out, N_TP)
    mixed = (residual.astype(jnp.float32) + projected).astype(jnp.bfloat16)
    normed = normalize(mixed, norm_gain)
    gate_proj = jnp.dot(normed, w_gate, preferred_element_type=jnp.float32)
    up_proj = jnp.dot(normed, w_up, preferred_element_type=jnp.float32)
    hidden = (jax.nn.silu(gate_proj) * up_proj).astype(jnp.bfloat16)
    down_sum = group_sum(hidden, w_down, N_TP)
    summed = mixed.astype(jnp.float32) + 0.5 * down_sum
    scaled = summed * lax.rsqrt(lax.optimization_barrier(jnp.mean(summed * summed, axis=-1, keepdims=True)) + 1e-06)
    return scaled.astype(jnp.bfloat16)
```

```python
import functools
import math

import jax
import jax.numpy as jnp
from jax import lax
from jax.experimental import pallas as pl
from jax.experimental.pallas import tpu as pltpu
from jax.sharding import PartitionSpec as P


def normalize(rows_in, gain):
    floats = rows_in.astype(jnp.float32)
    scaled = floats * lax.rsqrt(jnp.mean(floats * floats, axis=-1, keepdims=True) + 1e-06)
    return (scaled * gain).astype(jnp.bfloat16)


def attend(queries, keys, values, log_gates):
    row_count = queries.shape[0]
    head_count = log_gates.shape[1]
    head_width = queries.shape[1] // head_count
    score_scale = head_width ** (-0.5)
    first_row = lax.axis_index("sp") * row_count
    query_heads = queries.reshape(row_count, head_count, head_width)
    query_gates = log_gates.T
    query_positions = first_row + jnp.arange(row_count, dtype=jnp.int32)
    initial = (
        jnp.full((head_count, row_count), -1e30, jnp.float32),
        jnp.zeros((head_count, row_count), jnp.float32),
        jnp.zeros((head_count, row_count, head_width), jnp.float32),
    )
    carried = initial
    key_piece = lax.all_gather(keys.astype(jnp.float32), "sp", axis=0, tiled=True).astype(
        jnp.bfloat16
    )
    value_piece = lax.all_gather(values.astype(jnp.float32), "sp", axis=0, tiled=True).astype(
        jnp.bfloat16
    )
    gate_piece = lax.all_gather(log_gates, "sp", axis=0, tiled=True)
    length = key_piece.shape[0]
    block_rows = math.gcd(length, 2048)
    block_count = length // block_rows
    key_blocks = key_piece.reshape(block_count, block_rows, head_count, head_width)
    value_blocks = value_piece.reshape(block_count, block_rows, head_count, head_width)
    gate_blocks = gate_piece.reshape(block_count, block_rows, head_count)
    offsets = jnp.arange(block_count, dtype=jnp.int32) * block_rows

    def one_block(state, inputs):
        current_key_block, value_block, gate_block, offset = inputs

        def work(current):
            running_max, running_sum, accumulated = current
            scores = (
                jnp.einsum(
                    "qhd,khd->hqk",
                    query_heads,
                    current_key_block,
                    preferred_element_type=jnp.float32,
                )
                * score_scale
            )
            scores = scores + query_gates[:, :, None] - gate_block.T[:, None, :]
            key_positions = offset + jnp.arange(block_rows, dtype=jnp.int32)
            causal = (query_positions[:, None] >= key_positions[None, :])[None]
            scores = jnp.where(causal, scores, -1e30)
            new_max = jnp.maximum(running_max, jnp.max(scores, axis=-1))
            weights = jnp.where(causal, jnp.exp(scores - new_max[:, :, None]), 0.0)
            rescale = jnp.exp(running_max - new_max)
            running_sum = running_sum * rescale + jnp.sum(weights, axis=-1)
            product = jnp.einsum(
                "hqk,khd->hqd",
                weights.astype(jnp.bfloat16),
                value_block,
                preferred_element_type=jnp.float32,
            )
            accumulated = accumulated * rescale[:, :, None] + product
            return (new_max, running_sum, accumulated)

        state = lax.cond(offset <= first_row + row_count - 1, work, lambda current: current, state)
        return (state, None)

    carried, _ = lax.scan(one_block, carried, (key_blocks, value_blocks, gate_blocks, offsets))
    running_max, running_sum, accumulated = carried
    attended = accumulated / running_sum[:, :, None]
    return (
        attended.transpose(1, 0, 2).reshape(row_count, head_count * head_width).astype(jnp.bfloat16)
    )


def body(residual, queries, keys, values, log_gates, w_out, norm_gain, w_gate, w_up, w_down):
    attended = attend(queries, keys, values, log_gates)
    row_count = attended.shape[0]
    per_device = row_count // lax.axis_size("tp")
    my_first = lax.axis_index("tp") * per_device
    projected = lax.psum(
        jnp.dot(attended, w_out, preferred_element_type=jnp.float32).astype(jnp.bfloat16), "tp"
    ).astype(jnp.float32)
    mixed_all = (residual.astype(jnp.float32) + projected).astype(jnp.bfloat16)
    normed_all = normalize(mixed_all, norm_gain)
    mixed = lax.dynamic_slice_in_dim(mixed_all, my_first, per_device, 0)
    gate_whole = lax.all_gather(w_gate, "sp", axis=0, tiled=True)
    up_whole = lax.all_gather(w_up, "sp", axis=0, tiled=True)
    down_whole = lax.all_gather(w_down, "sp", axis=1, tiled=True)
    gate_proj = jnp.dot(normed_all, gate_whole, preferred_element_type=jnp.float32)
    up_proj = jnp.dot(normed_all, up_whole, preferred_element_type=jnp.float32)
    hidden = (jax.nn.silu(gate_proj) * up_proj).astype(jnp.bfloat16)
    down_sum = lax.psum_scatter(
        jnp.dot(hidden, down_whole, preferred_element_type=jnp.float32).astype(jnp.bfloat16),
        "tp",
        scatter_dimension=0,
        tiled=True,
    ).astype(jnp.float32)
    summed = mixed.astype(jnp.float32) + 0.5 * down_sum
    scaled = summed * lax.rsqrt(jnp.mean(summed * summed, axis=-1, keepdims=True) + 1e-06)
    return scaled.astype(jnp.bfloat16)


MESH = pl.DeviceIdType.MESH


def send(src, dst, sems, index, target):
    return pltpu.make_async_remote_copy(
        src_ref=src,
        dst_ref=dst,
        send_sem=sems.at[(0, *index)],
        recv_sem=sems.at[(1, *index)],
        device_id=target,
        device_id_type=MESH,
    )


def layer_kernel(
    n, tp, chunk,
    q_ref, k_ref, v_ref, g_ref, gt_ref, residual_ref, w_out_ref, gain_ref, wg_ref, wu_ref, wd_ref,
    out_ref,
    k_all, v_all, gt_all, att, proj, pc_buf, px_send, px_buf, mixed, normed,
    wg_all, wu_all, wd_all, hid, part, c_buf, x_send, x_buf, z_send, z_buf,
    kv_sems, w_sems, y_sems, pc_sems, px_sems, nz_sems, nx_sems, nc_sems, c_sems, x_sems, z_sems,
):
    me = lax.axis_index("sp")
    t = lax.axis_index("tp")
    g = lax.axis_index("grp")
    x, c = t // 2, t % 2
    nx = tp // 2
    mate = x * 2 + (1 - c)
    rows = q_ref.shape[0]
    sub = rows // tp
    width = residual_ref.shape[1]
    heads = g_ref.shape[1]
    head = q_ref.shape[1] // heads
    depth = wg_ref.shape[0]
    ff = wg_ref.shape[1]
    half = depth // 2
    dcols = wd_ref.shape[1]
    dhalf = dcols // 2

    def there(d):
        return lax.rem(me + d, n)

    def origin(d):
        return lax.rem(me + n - d, n)

    def across(dx):
        return lax.rem(x + dx, nx)

    barrier = pltpu.get_barrier_semaphore()
    for d in range(1, n):
        pl.semaphore_signal(barrier, inc=1, device_id={"sp": there(d)}, device_id_type=MESH)
    for dx in range(1, nx):
        pl.semaphore_signal(
            barrier, inc=1, device_id={"tp": across(dx) * 2 + c}, device_id_type=MESH
        )
    pl.semaphore_signal(barrier, inc=1, device_id={"tp": mate}, device_id_type=MESH)
    pl.semaphore_signal(barrier, inc=1, device_id={"grp": 1 - g}, device_id_type=MESH)
    pl.semaphore_wait(barrier, n - 1 + nx - 1 + 2)

    def kv_copies(d):
        target = {"sp": there(d)}
        return (
            send(k_ref, k_all.at[d - 1], kv_sems, (d - 1, 0), target),
            send(v_ref, v_all.at[d - 1], kv_sems, (d - 1, 1), target),
            send(gt_ref, gt_all.at[d - 1], kv_sems, (d - 1, 2), target),
        )

    for d in range(1, n):

        @pl.when(me + d < n)
        def _(d=d):
            for copy in kv_copies(d):
                copy.start()

    def w_copies(d):
        j = there(d)
        start = pl.multiple_of(jnp.minimum(j * chunk, ff - chunk), 128)
        target = {"sp": j}
        in_rows = pl.ds(pl.multiple_of(g * half, half), half)
        in_cols = pl.ds(pl.multiple_of(g * dhalf, dhalf), dhalf)
        return (
            send(wg_ref.at[in_rows, pl.ds(start, chunk)], wg_all.at[d, in_rows], w_sems, (d - 1, 0), target),
            send(wu_ref.at[in_rows, pl.ds(start, chunk)], wu_all.at[d, in_rows], w_sems, (d - 1, 1), target),
            send(wd_ref.at[pl.ds(start, chunk), in_cols], wd_all.at[d, :, in_cols], w_sems, (d - 1, 2), target),
        )

    def y_copies(d):
        target = {"grp": 1 - g}
        in_rows = pl.ds(pl.multiple_of(g * half, half), half)
        in_cols = pl.ds(pl.multiple_of(g * dhalf, dhalf), dhalf)
        return (
            send(wg_all.at[d, in_rows], wg_all.at[d, in_rows], y_sems, (d - 1, 0), target),
            send(wu_all.at[d, in_rows], wu_all.at[d, in_rows], y_sems, (d - 1, 1), target),
            send(wd_all.at[d, :, in_cols], wd_all.at[d, :, in_cols], y_sems, (d - 1, 2), target),
        )

    for d in range(1, n):
        for copy in w_copies(d):
            copy.start()

    mine = pl.multiple_of(jnp.minimum(me * chunk, ff - chunk), 128)
    wg_all[0] = wg_ref[:, pl.ds(mine, chunk)]
    wu_all[0] = wu_ref[:, pl.ds(mine, chunk)]
    wd_all[0] = wd_ref[pl.ds(mine, chunk), :]

    for d in range(1, n):

        @pl.when(me + d < n)
        def _(d=d):
            for copy in kv_copies(d):
                copy.wait_send()

        @pl.when(me >= d)
        def _(d=d):
            for copy in kv_copies(d):
                copy.wait_recv()

        @pl.when(me < d)
        def _(d=d):
            k_all[d - 1] = jnp.zeros_like(k_ref)
            v_all[d - 1] = jnp.zeros_like(v_ref)
            gt_all[d - 1] = jnp.zeros_like(gt_ref)

    pair = 128 // head
    lane = lax.broadcasted_iota(jnp.int32, (rows, 128), 1)
    causal = lax.broadcasted_iota(jnp.int32, (rows, rows), 0) >= lax.broadcasted_iota(
        jnp.int32, (rows, rows), 1
    )
    contract = (((1,), (1,)), ((), ()))
    for p in range(heads // pair):
        cols = slice(p * 128, (p + 1) * 128)
        q_pair = q_ref[:, cols]
        joined = jnp.zeros((rows, 128), jnp.float32)
        for i in range(pair):
            h = p * pair + i
            inside = (lane >= i * head) & (lane < (i + 1) * head)
            q_head = jnp.where(inside, q_pair, jnp.zeros_like(q_pair))
            g_query = g_ref[:, h : h + 1]
            scores = []
            for d in range(n):
                k_pair = k_ref[:, cols] if d == 0 else k_all[d - 1, :, cols]
                g_key = gt_ref[h : h + 1, :] if d == 0 else gt_all[d - 1, h : h + 1, :]
                score = (
                    lax.dot_general(q_head, k_pair, contract, preferred_element_type=jnp.float32)
                    * head ** (-0.5)
                    + g_query
                    - g_key
                )
                allowed = causal if d == 0 else (jnp.zeros((rows, rows), jnp.int32) + me) >= d
                scores.append(jnp.where(allowed, score, -1e30))
            peak = functools.reduce(
                jnp.maximum, [jnp.max(score, axis=-1, keepdims=True) for score in scores]
            )
            total = jnp.zeros((rows, 1), jnp.float32)
            summed = jnp.zeros((rows, 128), jnp.float32)
            for d in range(n):
                v_pair = v_ref[:, cols] if d == 0 else v_all[d - 1, :, cols]
                weight = jnp.exp(scores[d] - peak)
                total += jnp.sum(weight, axis=-1, keepdims=True)
                summed += jnp.dot(
                    weight.astype(jnp.bfloat16), v_pair, preferred_element_type=jnp.float32
                )
            joined = jnp.where(inside, summed / total, joined)
        att[:, cols] = joined.astype(jnp.bfloat16)

    for k in range(width // 512):
        cols = slice(k * 512, (k + 1) * 512)
        proj[:, cols] = jnp.dot(
            att[...], w_out_ref[:, cols], preferred_element_type=jnp.float32
        ).astype(jnp.bfloat16)

    def block(index):
        return pl.ds(pl.multiple_of(index * sub, sub), sub)

    pc = [
        send(proj.at[block(across(dx) * 2 + 1 - c)], pc_buf.at[dx], pc_sems, (dx,), {"tp": mate})
        for dx in range(nx)
    ]
    for copy in pc:
        copy.start()
    px = [
        send(px_send.at[dx], px_buf.at[dx], px_sems, (dx,), {"tp": across(dx) * 2 + c})
        for dx in range(nx)
    ]
    for dx in range(1, nx):
        pc[dx].wait_recv()
        px_send[dx] = (
            proj[block(across(dx) * 2 + c), :].astype(jnp.float32) + pc_buf[dx].astype(jnp.float32)
        ).astype(jnp.bfloat16)
        px[dx].start()
    pc[0].wait_recv()
    acc = proj[block(t), :].astype(jnp.float32) + pc_buf[0].astype(jnp.float32)
    for dx in range(1, nx):
        px[dx].wait_recv()
        acc += px_buf[dx].astype(jnp.float32)
    mix = (residual_ref[block(t), :].astype(jnp.float32) + acc).astype(jnp.bfloat16)
    mixed[...] = mix
    floats = mix.astype(jnp.float32)
    scale = lax.rsqrt(jnp.mean(floats * floats, axis=-1, keepdims=True) + 1e-06)
    normed[me, block(t), :] = (floats * scale * gain_ref[...]).astype(jnp.bfloat16)

    own = normed.at[me, block(t)]
    nz = [send(own, own, nz_sems, (d,), {"sp": there(d)}) for d in range(n)]
    for d in range(1, n):
        nz[d].start()

    def spread(d):
        piece = normed.at[origin(d), block(t)]
        copies = [send(piece, piece, nc_sems, (d, 0), {"tp": mate})]
        for dx in range(1, nx):
            copies.append(send(piece, piece, nx_sems, (d, dx), {"tp": across(dx) * 2 + c}))
        return copies

    def relay(d, dx):
        piece = normed.at[origin(d), block(lax.rem(x + nx - dx, nx) * 2 + c)]
        return send(piece, piece, nc_sems, (d, dx), {"tp": mate})

    spreads = [spread(d) for d in range(n)]
    for copy in spreads[0]:
        copy.start()
    for d in range(1, n):
        for copy, forward in zip(w_copies(d), y_copies(d)):
            copy.wait_recv()
            forward.start()
    for dx in range(1, nx):
        spreads[0][dx].wait_recv()
        relay(0, dx).start()
    for d in range(1, n):
        nz[d].wait_recv()
        for copy in spreads[d]:
            copy.start()
    for d in range(1, n):
        for dx in range(1, nx):
            spreads[d][dx].wait_recv()
            relay(d, dx).start()
    for d in range(1, n):
        for copy in y_copies(d):
            copy.wait_recv()
    for d in range(n):
        spreads[d][0].wait_recv()
        for dx in range(1, nx):
            relay(d, dx).wait_recv()

    skipped = me * chunk - mine
    live = lax.broadcasted_iota(jnp.int32, (rows, chunk), 1) >= skipped
    order = [d % n for d in range(1, n + 1)]

    def c_copy(d, dx):
        j = there(d)
        return send(
            part.at[j, block(across(dx) * 2 + 1 - c)], c_buf.at[d, dx], c_sems, (d, dx), {"tp": mate}
        )

    def feed(index, carry):
        d = lax.rem(index + 1, n)
        j = there(d)
        gate = jnp.zeros((rows, chunk), jnp.float32)
        up = jnp.zeros((rows, chunk), jnp.float32)
        for e in range(n):
            piece = normed[j, :, pl.ds(pl.multiple_of(origin(e) * depth, depth), depth)]
            gate += jnp.dot(piece, wg_all[e], preferred_element_type=jnp.float32)
            up += jnp.dot(piece, wu_all[e], preferred_element_type=jnp.float32)
        value = gate / (1.0 + jnp.exp(-gate)) * up
        hid[...] = jnp.where(live, value, 0.0).astype(jnp.bfloat16)
        for e in range(n):
            part[j, :, pl.ds(pl.multiple_of(origin(e) * dcols, dcols), dcols)] = jnp.dot(
                hid[...], wd_all[e], preferred_element_type=jnp.float32
            ).astype(jnp.bfloat16)
        for dx in range(nx):
            c_copy(d, dx).start()
        return carry

    lax.fori_loop(0, n, feed, 0)

    def x_copy(d, dx):
        return send(x_send.at[d, dx], x_buf.at[d, dx], x_sems, (d, dx), {"tp": across(dx) * 2 + c})

    def z_copy(d):
        return send(z_send.at[d], z_buf.at[d], z_sems, (d,), {"sp": there(d)})

    for d in order:
        for dx in range(1, nx):
            c_copy(d, dx).wait_recv()
            x_send[d, dx] = (
                part[there(d), block(across(dx) * 2 + c), :].astype(jnp.float32)
                + c_buf[d, dx].astype(jnp.float32)
            ).astype(jnp.bfloat16)
            x_copy(d, dx).start()
    for d in order:
        c_copy(d, 0).wait_recv()
        acc = part[there(d), block(t), :].astype(jnp.float32) + c_buf[d, 0].astype(jnp.float32)
        for dx in range(1, nx):
            x_copy(d, dx).wait_recv()
            acc += x_buf[d, dx].astype(jnp.float32)
        if d != 0:
            z_send[d] = acc.astype(jnp.bfloat16)
            z_copy(d).start()
    for d in range(1, n):
        z_copy(d).wait_recv()
        acc += z_buf[d].astype(jnp.float32)
    summed = mixed[...].astype(jnp.float32) + 0.5 * acc
    scale = lax.rsqrt(jnp.mean(summed * summed, axis=-1, keepdims=True) + 1e-06)
    out_ref[...] = (summed * scale).astype(jnp.bfloat16)

    for copy in pc:
        copy.wait_send()
    for dx in range(1, nx):
        px[dx].wait_send()
    for d in range(n):
        for copy in spreads[d]:
            copy.wait_send()
        for dx in range(1, nx):
            relay(d, dx).wait_send()
            x_copy(d, dx).wait_send()
        for dx in range(nx):
            c_copy(d, dx).wait_send()
    for d in range(1, n):
        nz[d].wait_send()
        z_copy(d).wait_send()
        for copy in w_copies(d):
            copy.wait_send()
        for copy in y_copies(d):
            copy.wait_send()


def fused_body(residual, queries, keys, values, log_gates, w_out, norm_gain, w_gate, w_up, w_down):
    n, tp = lax.axis_size("sp"), lax.axis_size("tp")
    rows, width = residual.shape
    sub = rows // tp
    nx = tp // 2
    heads = log_gates.shape[1]
    depth, ff = w_gate.shape
    dcols = w_down.shape[1]
    chunk = window(ff, n)
    gates_t = jnp.pad(log_gates.T, ((0, -heads % 8), (0, 0)))
    bf16, f32 = jnp.bfloat16, jnp.float32
    shapes = [
        ((n - 1, *keys.shape), bf16),
        ((n - 1, *values.shape), bf16),
        ((n - 1, *gates_t.shape), f32),
        (queries.shape, bf16),
        ((rows, width), bf16),
        ((nx, sub, width), bf16),
        ((nx, sub, width), bf16),
        ((nx, sub, width), bf16),
        ((sub, width), bf16),
        ((n, rows, width), bf16),
        ((n, depth, chunk), bf16),
        ((n, depth, chunk), bf16),
        ((n, chunk, dcols), bf16),
        ((rows, chunk), bf16),
        ((n, rows, width), bf16),
        ((n, nx, sub, width), bf16),
        ((n, nx, sub, width), bf16),
        ((n, nx, sub, width), bf16),
        ((n, sub, width), bf16),
        ((n, sub, width), bf16),
    ]
    sems = [
        (2, n - 1, 3),
        (2, n - 1, 3),
        (2, n - 1, 3),
        (2, nx),
        (2, nx),
        (2, n),
        (2, n, nx),
        (2, n, nx),
        (2, n, nx),
        (2, n, nx),
        (2, n),
    ]
    return pl.pallas_call(
        functools.partial(layer_kernel, n, tp, chunk),
        out_shape=jax.ShapeDtypeStruct((sub, width), bf16),
        in_specs=[pl.BlockSpec(memory_space=pltpu.VMEM)] * 11,
        out_specs=pl.BlockSpec(memory_space=pltpu.VMEM),
        scratch_shapes=[pltpu.VMEM(shape, dtype) for shape, dtype in shapes]
        + [pltpu.SemaphoreType.DMA(shape) for shape in sems],
        compiler_params=pltpu.CompilerParams(
            collective_id=0, has_side_effects=True, vmem_limit_bytes=60 * 1024 * 1024
        ),
    )(
        queries, keys, values, log_gates, gates_t, residual, w_out, norm_gain[None, :],
        w_gate, w_up, w_down,
    )


def window(ff, n):
    return -(-ff // (n * 128)) * 128


def fits(mesh, shapes):
    residual, queries, gates, gate = shapes
    n, tp, grp = mesh.shape["sp"], mesh.shape["tp"], mesh.shape["grp"]
    ff = gate[1] // tp
    heads = gates[1] // tp
    head = queries[1] // gates[1]
    rows = residual[0] // (grp * n)
    return (
        grp == 2
        and 2 <= n <= 4
        and tp % 2 == 0
        and ff % 128 == 0
        and window(ff, n) * (n - 1) < ff
        and 128 % head == 0
        and (heads * head) % 128 == 0
        and rows % (16 * tp) == 0
        and rows * n * residual[1] <= 1 << 21
    )


def solution(mesh):
    in_specs = (
        P(("grp", "sp"), None),
        P(("grp", "sp"), "tp"),
        P(("grp", "sp"), "tp"),
        P(("grp", "sp"), "tp"),
        P(("grp", "sp"), "tp"),
        P("tp", None),
        P(),
        P("sp", "tp"),
        P("sp", "tp"),
        P("tp", "sp"),
    )
    out_specs = P(("grp", "sp", "tp"), None)

    def layer(*args):
        residual, queries, _, _, log_gates, _, _, w_gate, _, _ = args
        shapes = (residual.shape, queries.shape, log_gates.shape, w_gate.shape)
        chosen = fused_body if fits(mesh, shapes) else body
        return jax.shard_map(
            chosen, mesh=mesh, in_specs=in_specs, out_specs=out_specs, check_vma=False
        )(*args)

    return layer
```

```python
import functools
import math

import jax
import jax.numpy as jnp
from jax import lax
from jax.experimental import pallas as pl
from jax.experimental.pallas import tpu as pltpu
from jax.sharding import PartitionSpec as P


def normalize(rows_in, gain):
    floats = rows_in.astype(jnp.float32)
    scaled = floats * lax.rsqrt(jnp.mean(floats * floats, axis=-1, keepdims=True) + 1e-06)
    return (scaled * gain).astype(jnp.bfloat16)


def attend(queries, keys, values, log_gates):
    row_count = queries.shape[0]
    head_count = log_gates.shape[1]
    head_width = queries.shape[1] // head_count
    score_scale = head_width ** (-0.5)
    first_row = lax.axis_index("sp") * row_count
    query_heads = queries.reshape(row_count, head_count, head_width)
    query_gates = log_gates.T
    query_positions = first_row + jnp.arange(row_count, dtype=jnp.int32)
    initial = (
        jnp.full((head_count, row_count), -1e30, jnp.float32),
        jnp.zeros((head_count, row_count), jnp.float32),
        jnp.zeros((head_count, row_count, head_width), jnp.float32),
    )
    carried = initial
    key_piece = lax.all_gather(keys.astype(jnp.float32), "sp", axis=0, tiled=True).astype(
        jnp.bfloat16
    )
    value_piece = lax.all_gather(values.astype(jnp.float32), "sp", axis=0, tiled=True).astype(
        jnp.bfloat16
    )
    gate_piece = lax.all_gather(log_gates, "sp", axis=0, tiled=True)
    length = key_piece.shape[0]
    block_rows = math.gcd(length, 2048)
    block_count = length // block_rows
    key_blocks = key_piece.reshape(block_count, block_rows, head_count, head_width)
    value_blocks = value_piece.reshape(block_count, block_rows, head_count, head_width)
    gate_blocks = gate_piece.reshape(block_count, block_rows, head_count)
    offsets = jnp.arange(block_count, dtype=jnp.int32) * block_rows

    def one_block(state, inputs):
        current_key_block, value_block, gate_block, offset = inputs

        def work(current):
            running_max, running_sum, accumulated = current
            scores = (
                jnp.einsum(
                    "qhd,khd->hqk",
                    query_heads,
                    current_key_block,
                    preferred_element_type=jnp.float32,
                )
                * score_scale
            )
            scores = scores + query_gates[:, :, None] - gate_block.T[:, None, :]
            key_positions = offset + jnp.arange(block_rows, dtype=jnp.int32)
            causal = (query_positions[:, None] >= key_positions[None, :])[None]
            scores = jnp.where(causal, scores, -1e30)
            new_max = jnp.maximum(running_max, jnp.max(scores, axis=-1))
            weights = jnp.where(causal, jnp.exp(scores - new_max[:, :, None]), 0.0)
            rescale = jnp.exp(running_max - new_max)
            running_sum = running_sum * rescale + jnp.sum(weights, axis=-1)
            product = jnp.einsum(
                "hqk,khd->hqd",
                weights.astype(jnp.bfloat16),
                value_block,
                preferred_element_type=jnp.float32,
            )
            accumulated = accumulated * rescale[:, :, None] + product
            return (new_max, running_sum, accumulated)

        state = lax.cond(offset <= first_row + row_count - 1, work, lambda current: current, state)
        return (state, None)

    carried, _ = lax.scan(one_block, carried, (key_blocks, value_blocks, gate_blocks, offsets))
    running_max, running_sum, accumulated = carried
    attended = accumulated / running_sum[:, :, None]
    return (
        attended.transpose(1, 0, 2).reshape(row_count, head_count * head_width).astype(jnp.bfloat16)
    )


def body(residual, queries, keys, values, log_gates, w_out, norm_gain, w_gate, w_up, w_down):
    attended = attend(queries, keys, values, log_gates)
    row_count = attended.shape[0]
    per_device = row_count // lax.axis_size("tp")
    my_first = lax.axis_index("tp") * per_device
    projected = lax.psum(
        jnp.dot(attended, w_out, preferred_element_type=jnp.float32).astype(jnp.bfloat16), "tp"
    ).astype(jnp.float32)
    mixed_all = (residual.astype(jnp.float32) + projected).astype(jnp.bfloat16)
    normed_all = normalize(mixed_all, norm_gain)
    mixed = lax.dynamic_slice_in_dim(mixed_all, my_first, per_device, 0)
    gate_whole = lax.all_gather(w_gate, "sp", axis=0, tiled=True)
    up_whole = lax.all_gather(w_up, "sp", axis=0, tiled=True)
    down_whole = lax.all_gather(w_down, "sp", axis=1, tiled=True)
    gate_proj = jnp.dot(normed_all, gate_whole, preferred_element_type=jnp.float32)
    up_proj = jnp.dot(normed_all, up_whole, preferred_element_type=jnp.float32)
    hidden = (jax.nn.silu(gate_proj) * up_proj).astype(jnp.bfloat16)
    down_sum = lax.psum_scatter(
        jnp.dot(hidden, down_whole, preferred_element_type=jnp.float32).astype(jnp.bfloat16),
        "tp",
        scatter_dimension=0,
        tiled=True,
    ).astype(jnp.float32)
    summed = mixed.astype(jnp.float32) + 0.5 * down_sum
    scaled = summed * lax.rsqrt(jnp.mean(summed * summed, axis=-1, keepdims=True) + 1e-06)
    return scaled.astype(jnp.bfloat16)


MESH = pl.DeviceIdType.MESH


def send(src, dst, sems, index, target):
    return pltpu.make_async_remote_copy(
        src_ref=src,
        dst_ref=dst,
        send_sem=sems.at[(0, *index)],
        recv_sem=sems.at[(1, *index)],
        device_id=target,
        device_id_type=MESH,
    )


def layer_kernel(
    n, tp, chunk,
    q_ref, k_ref, v_ref, g_ref, gt_ref, residual_ref, w_out_ref, gain_ref, wg_ref, wu_ref, wd_ref,
    out_ref,
    k_all, v_all, gt_all, att, proj, pc_buf, px_send, px_buf, mixed, normed,
    wg_all, wu_all, wd_all, hid, part, c_buf, x_send, x_buf, z_send, z_buf,
    kv_sems, w_sems, y_sems, pc_sems, px_sems, nz_sems, nx_sems, nc_sems, c_sems, x_sems, z_sems,
):
    me = lax.axis_index("sp")
    t = lax.axis_index("tp")
    g = lax.axis_index("grp")
    x, c = t // 2, t % 2
    nx = tp // 2
    mate = x * 2 + (1 - c)
    rows = q_ref.shape[0]
    sub = rows // tp
    width = residual_ref.shape[1]
    heads = g_ref.shape[1]
    head = q_ref.shape[1] // heads
    depth = wg_ref.shape[0]
    ff = wg_ref.shape[1]
    half = depth // 2
    dcols = wd_ref.shape[1]
    dhalf = dcols // 2

    def there(d):
        return lax.rem(me + d, n)

    def origin(d):
        return lax.rem(me + n - d, n)

    def across(dx):
        return lax.rem(x + dx, nx)

    barrier = pltpu.get_barrier_semaphore()
    for d in range(1, n):
        pl.semaphore_signal(barrier, inc=1, device_id={"sp": there(d)}, device_id_type=MESH)
    for dx in range(1, nx):
        pl.semaphore_signal(
            barrier, inc=1, device_id={"tp": across(dx) * 2 + c}, device_id_type=MESH
        )
    pl.semaphore_signal(barrier, inc=1, device_id={"tp": mate}, device_id_type=MESH)
    pl.semaphore_signal(barrier, inc=1, device_id={"grp": 1 - g}, device_id_type=MESH)
    pl.semaphore_wait(barrier, n - 1 + nx - 1 + 2)

    def kv_copies(d):
        target = {"sp": lax.rem(me + 1, n)}
        own = (k_ref, v_ref, gt_ref)
        held = (k_all, v_all, gt_all)
        return [
            send(
                own[i] if d == 1 else held[i].at[d - 2], held[i].at[d - 1], kv_sems, (d - 1, i), target
            )
            for i in range(3)
        ]

    @pl.when(me + 1 < n)
    def _():
        for copy in kv_copies(1):
            copy.start()

    last = ff - (n - 1) * chunk
    my_rows = pl.ds(pl.multiple_of(g * half, half), half)
    my_cols = pl.ds(pl.multiple_of(g * dhalf, dhalf), dhalf)

    def w_copies(d, size):
        j = there(d)
        place = pl.ds(pl.multiple_of(jnp.minimum(j * chunk, ff - size), 128), size)
        target = {"sp": j}
        return (
            send(wg_ref.at[my_rows, place], wg_all.at[d, my_rows, :size], w_sems, (d - 1, 0), target),
            send(wu_ref.at[my_rows, place], wu_all.at[d, my_rows, :size], w_sems, (d - 1, 1), target),
            send(wd_ref.at[place, my_cols], wd_all.at[d, :size, my_cols], w_sems, (d - 1, 2), target),
        )

    def y_copies(d, size):
        target = {"grp": 1 - g}
        gate = wg_all.at[d, my_rows, :size]
        up = wu_all.at[d, my_rows, :size]
        down = wd_all.at[d, :size, my_cols]
        return (
            send(gate, gate, y_sems, (d - 1, 0), target),
            send(up, up, y_sems, (d - 1, 1), target),
            send(down, down, y_sems, (d - 1, 2), target),
        )

    def by_window(owner, work):
        pl.when(owner < n - 1)(lambda: work(chunk))
        pl.when(owner == n - 1)(lambda: work(last))

    def start_weights(d):
        def work(size):
            for copy in w_copies(d, size):
                copy.start()

        by_window(there(d), work)

    def pass_weights(d):
        def work(size):
            for copy, forward in zip(w_copies(d, size), y_copies(d, size)):
                copy.wait_recv()
                forward.start()

        by_window(me, work)

    for d in range(1, n):

        @pl.when(me + d >= n)
        def _(d=d):
            start_weights(d)

    def own_weights(size):
        mine = pl.ds(pl.multiple_of(me * chunk, 128), size)
        wg_all[0, :, :size] = wg_ref[:, mine]
        wu_all[0, :, :size] = wu_ref[:, mine]
        wd_all[0, :size, :] = wd_ref[mine, :]
        if size < chunk:
            for d in range(n):
                wg_all[d, :, size:] = jnp.zeros((depth, chunk - size), jnp.bfloat16)
                wu_all[d, :, size:] = jnp.zeros((depth, chunk - size), jnp.bfloat16)
                wd_all[d, size:, :] = jnp.zeros((chunk - size, dcols), jnp.bfloat16)

    by_window(me, own_weights)

    for d in range(1, n):
        if d == n - 1:
            for e in range(1, n):

                @pl.when(me + e < n)
                def _(e=e):
                    start_weights(e)

        @pl.when(me >= d)
        def _(d=d):
            arrived = kv_copies(d)
            forwards = kv_copies(d + 1) if d + 1 < n else [None] * 3
            for copy, forward in zip(arrived, forwards):
                copy.wait_recv()
                if forward is not None:
                    pl.when(me + 1 < n)(forward.start)

        @pl.when(me < d)
        def _(d=d):
            k_all[d - 1] = jnp.zeros_like(k_ref)
            v_all[d - 1] = jnp.zeros_like(v_ref)
            gt_all[d - 1] = jnp.zeros_like(gt_ref)

    pair = 128 // head
    lane = lax.broadcasted_iota(jnp.int32, (rows, 128), 1)
    causal = lax.broadcasted_iota(jnp.int32, (rows, rows), 0) >= lax.broadcasted_iota(
        jnp.int32, (rows, rows), 1
    )
    contract = (((1,), (1,)), ((), ()))
    for p in range(heads // pair):
        cols = slice(p * 128, (p + 1) * 128)
        q_pair = q_ref[:, cols]
        joined = jnp.zeros((rows, 128), jnp.float32)
        for i in range(pair):
            h = p * pair + i
            inside = (lane >= i * head) & (lane < (i + 1) * head)
            q_head = jnp.where(inside, q_pair, jnp.zeros_like(q_pair))
            g_query = g_ref[:, h : h + 1]
            scores = []
            for d in range(n):
                k_pair = k_ref[:, cols] if d == 0 else k_all[d - 1, :, cols]
                g_key = gt_ref[h : h + 1, :] if d == 0 else gt_all[d - 1, h : h + 1, :]
                score = (
                    lax.dot_general(q_head, k_pair, contract, preferred_element_type=jnp.float32)
                    * head ** (-0.5)
                    + g_query
                    - g_key
                )
                allowed = causal if d == 0 else (jnp.zeros((rows, rows), jnp.int32) + me) >= d
                scores.append(jnp.where(allowed, score, -1e30))
            peak = functools.reduce(
                jnp.maximum, [jnp.max(score, axis=-1, keepdims=True) for score in scores]
            )
            total = jnp.zeros((rows, 1), jnp.float32)
            summed = jnp.zeros((rows, 128), jnp.float32)
            for d in range(n):
                v_pair = v_ref[:, cols] if d == 0 else v_all[d - 1, :, cols]
                weight = jnp.exp(scores[d] - peak)
                total += jnp.sum(weight, axis=-1, keepdims=True)
                summed += jnp.dot(
                    weight.astype(jnp.bfloat16), v_pair, preferred_element_type=jnp.float32
                )
            joined = jnp.where(inside, summed / total, joined)
        att[:, cols] = joined.astype(jnp.bfloat16)

    pass_weights(1)
    for k in range(width // 512):
        cols = slice(k * 512, (k + 1) * 512)
        proj[:, cols] = jnp.dot(
            att[...], w_out_ref[:, cols], preferred_element_type=jnp.float32
        ).astype(jnp.bfloat16)

    def block(index):
        return pl.ds(pl.multiple_of(index * sub, sub), sub)

    pc = [
        send(proj.at[block(across(dx) * 2 + 1 - c)], pc_buf.at[dx], pc_sems, (dx,), {"tp": mate})
        for dx in range(nx)
    ]
    for copy in pc:
        copy.start()
    px = [
        send(px_send.at[dx], px_buf.at[dx], px_sems, (dx,), {"tp": across(dx) * 2 + c})
        for dx in range(nx)
    ]
    for dx in range(1, nx):
        pc[dx].wait_recv()
        px_send[dx] = (
            proj[block(across(dx) * 2 + c), :].astype(jnp.float32) + pc_buf[dx].astype(jnp.float32)
        ).astype(jnp.bfloat16)
        px[dx].start()
    if n > 2:
        pass_weights(2)
    pc[0].wait_recv()
    acc = proj[block(t), :].astype(jnp.float32) + pc_buf[0].astype(jnp.float32)
    for dx in range(1, nx):
        px[dx].wait_recv()
        acc += px_buf[dx].astype(jnp.float32)
    mix = (residual_ref[block(t), :].astype(jnp.float32) + acc).astype(jnp.bfloat16)
    mixed[...] = mix
    floats = mix.astype(jnp.float32)
    scale = lax.rsqrt(jnp.mean(floats * floats, axis=-1, keepdims=True) + 1e-06)
    normed[me, block(t), :] = (floats * scale * gain_ref[...]).astype(jnp.bfloat16)

    own = normed.at[me, block(t)]
    nz = [send(own, own, nz_sems, (d,), {"sp": there(d)}) for d in range(n)]
    for d in range(1, n):
        nz[d].start()

    def spread(d):
        piece = normed.at[origin(d), block(t)]
        copies = [send(piece, piece, nc_sems, (d, 0), {"tp": mate})]
        for dx in range(1, nx):
            copies.append(send(piece, piece, nx_sems, (d, dx), {"tp": across(dx) * 2 + c}))
        return copies

    def relay(d, dx):
        piece = normed.at[origin(d), block(lax.rem(x + nx - dx, nx) * 2 + c)]
        return send(piece, piece, nc_sems, (d, dx), {"tp": mate})

    spreads = [spread(d) for d in range(n)]
    for copy in spreads[0]:
        copy.start()
    for d in range(3, n):
        pass_weights(d)

    def relay_all(d):
        for dx in range(1, nx):
            spreads[d][dx].wait_recv()
            relay(d, dx).start()

    relay_all(0)
    for d in range(1, n):
        nz[d].wait_recv()
        for copy in spreads[d]:
            copy.start()
        if d > 1:
            relay_all(d - 1)

    def y_arrived(size):
        for d in range(1, n):
            for copy in y_copies(d, size):
                copy.wait_recv()

    by_window(me, y_arrived)

    def c_copy(d, dx):
        j = origin(d)
        return send(
            part.at[j, block(across(dx) * 2 + 1 - c)], c_buf.at[d, dx], c_sems, (d, dx), {"tp": mate}
        )

    def feed(d):
        j = origin(d)
        spreads[d][0].wait_recv()
        for dx in range(1, nx):
            relay(d, dx).wait_recv()
        gate = jnp.zeros((rows, chunk), jnp.float32)
        up = jnp.zeros((rows, chunk), jnp.float32)
        for e in range(n):
            piece = normed[j, :, pl.ds(pl.multiple_of(origin(e) * depth, depth), depth)]
            gate += jnp.dot(piece, wg_all[e], preferred_element_type=jnp.float32)
            up += jnp.dot(piece, wu_all[e], preferred_element_type=jnp.float32)
        hid[...] = (gate / (1.0 + jnp.exp(-gate)) * up).astype(jnp.bfloat16)
        for e in range(n):
            part[j, :, pl.ds(pl.multiple_of(origin(e) * dcols, dcols), dcols)] = jnp.dot(
                hid[...], wd_all[e], preferred_element_type=jnp.float32
            ).astype(jnp.bfloat16)
        for dx in range(nx):
            c_copy(d, dx).start()

    def x_copy(d, dx):
        return send(x_send.at[d, dx], x_buf.at[d, dx], x_sems, (d, dx), {"tp": across(dx) * 2 + c})

    def z_copy(d):
        return send(z_send.at[d], z_buf.at[d], z_sems, (d,), {"sp": origin(d)})

    def over_x(d):
        for dx in range(1, nx):
            c_copy(d, dx).wait_recv()
            x_send[d, dx] = (
                part[origin(d), block(across(dx) * 2 + c), :].astype(jnp.float32)
                + c_buf[d, dx].astype(jnp.float32)
            ).astype(jnp.bfloat16)
            x_copy(d, dx).start()

    def over_z(d):
        c_copy(d, 0).wait_recv()
        acc = part[origin(d), block(t), :].astype(jnp.float32) + c_buf[d, 0].astype(jnp.float32)
        for dx in range(1, nx):
            x_copy(d, dx).wait_recv()
            acc += x_buf[d, dx].astype(jnp.float32)
        if d != 0:
            z_send[d] = acc.astype(jnp.bfloat16)
            z_copy(d).start()
        return acc

    for d in range(n):
        if d == n - 1:
            relay_all(d)
        feed(d)
        if d > 0:
            over_x(d - 1)
        if d > 2:
            over_z(d - 2)
    over_x(n - 1)
    for d in range(max(1, n - 2), n):
        over_z(d)
    acc = over_z(0)
    for d in range(1, n):
        z_copy(d).wait_recv()
        acc += z_buf[d].astype(jnp.float32)
    summed = mixed[...].astype(jnp.float32) + 0.5 * acc
    scale = lax.rsqrt(jnp.mean(summed * summed, axis=-1, keepdims=True) + 1e-06)
    out_ref[...] = (summed * scale).astype(jnp.bfloat16)

    for copy in pc:
        copy.wait_send()
    for dx in range(1, nx):
        px[dx].wait_send()
    for d in range(n):
        for copy in spreads[d]:
            copy.wait_send()
        for dx in range(1, nx):
            relay(d, dx).wait_send()
            x_copy(d, dx).wait_send()
        for dx in range(nx):
            c_copy(d, dx).wait_send()
    for d in range(1, n):
        nz[d].wait_send()
        z_copy(d).wait_send()

        def w_sent(size, d=d):
            for copy in w_copies(d, size):
                copy.wait_send()

        def y_sent(size, d=d):
            for copy in y_copies(d, size):
                copy.wait_send()

        by_window(there(d), w_sent)
        by_window(me, y_sent)

        @pl.when((me >= d - 1) & (me + 1 < n))
        def _(d=d):
            for copy in kv_copies(d):
                copy.wait_send()


def fused_body(residual, queries, keys, values, log_gates, w_out, norm_gain, w_gate, w_up, w_down):
    n, tp = lax.axis_size("sp"), lax.axis_size("tp")
    rows, width = residual.shape
    sub = rows // tp
    nx = tp // 2
    heads = log_gates.shape[1]
    depth, ff = w_gate.shape
    dcols = w_down.shape[1]
    chunk = window(ff, n)
    gates_t = jnp.pad(log_gates.T, ((0, -heads % 8), (0, 0)))
    bf16, f32 = jnp.bfloat16, jnp.float32
    shapes = [
        ((n - 1, *keys.shape), bf16),
        ((n - 1, *values.shape), bf16),
        ((n - 1, *gates_t.shape), f32),
        (queries.shape, bf16),
        ((rows, width), bf16),
        ((nx, sub, width), bf16),
        ((nx, sub, width), bf16),
        ((nx, sub, width), bf16),
        ((sub, width), bf16),
        ((n, rows, width), bf16),
        ((n, depth, chunk), bf16),
        ((n, depth, chunk), bf16),
        ((n, chunk, dcols), bf16),
        ((rows, chunk), bf16),
        ((n, rows, width), bf16),
        ((n, nx, sub, width), bf16),
        ((n, nx, sub, width), bf16),
        ((n, nx, sub, width), bf16),
        ((n, sub, width), bf16),
        ((n, sub, width), bf16),
    ]
    sems = [
        (2, n - 1, 3),
        (2, n - 1, 3),
        (2, n - 1, 3),
        (2, nx),
        (2, nx),
        (2, n),
        (2, n, nx),
        (2, n, nx),
        (2, n, nx),
        (2, n, nx),
        (2, n),
    ]
    return pl.pallas_call(
        functools.partial(layer_kernel, n, tp, chunk),
        out_shape=jax.ShapeDtypeStruct((sub, width), bf16),
        in_specs=[pl.BlockSpec(memory_space=pltpu.VMEM)] * 11,
        out_specs=pl.BlockSpec(memory_space=pltpu.VMEM),
        scratch_shapes=[pltpu.VMEM(shape, dtype) for shape, dtype in shapes]
        + [pltpu.SemaphoreType.DMA(shape) for shape in sems],
        compiler_params=pltpu.CompilerParams(
            collective_id=0, has_side_effects=True, vmem_limit_bytes=60 * 1024 * 1024
        ),
    )(
        queries, keys, values, log_gates, gates_t, residual, w_out, norm_gain[None, :],
        w_gate, w_up, w_down,
    )


def window(ff, n):
    return -(-ff // (n * 128)) * 128


def fits(mesh, shapes):
    residual, queries, gates, gate = shapes
    n, tp, grp = mesh.shape["sp"], mesh.shape["tp"], mesh.shape["grp"]
    ff = gate[1] // tp
    heads = gates[1] // tp
    head = queries[1] // gates[1]
    rows = residual[0] // (grp * n)
    return (
        grp == 2
        and 2 <= n <= 4
        and tp % 2 == 0
        and ff % 128 == 0
        and window(ff, n) * (n - 1) < ff
        and 128 % head == 0
        and (heads * head) % 128 == 0
        and rows % (16 * tp) == 0
        and rows * n * residual[1] <= 1 << 21
    )


def solution(mesh):
    in_specs = (
        P(("grp", "sp"), None),
        P(("grp", "sp"), "tp"),
        P(("grp", "sp"), "tp"),
        P(("grp", "sp"), "tp"),
        P(("grp", "sp"), "tp"),
        P("tp", None),
        P(),
        P("sp", "tp"),
        P("sp", "tp"),
        P("tp", "sp"),
    )
    out_specs = P(("grp", "sp", "tp"), None)

    def layer(*args):
        residual, queries, _, _, log_gates, _, _, w_gate, _, _ = args
        shapes = (residual.shape, queries.shape, log_gates.shape, w_gate.shape)
        chosen = fused_body if fits(mesh, shapes) else body
        return jax.shard_map(
            chosen, mesh=mesh, in_specs=in_specs, out_specs=out_specs, check_vma=False
        )(*args)

    return layer
```

```python
import functools
import math

import jax
import jax.numpy as jnp
from jax import lax
from jax.experimental import pallas as pl
from jax.experimental.pallas import tpu as pltpu
from jax.sharding import PartitionSpec as P


def normalize(rows_in, gain):
    floats = rows_in.astype(jnp.float32)
    scaled = floats * lax.rsqrt(jnp.mean(floats * floats, axis=-1, keepdims=True) + 1e-06)
    return (scaled * gain).astype(jnp.bfloat16)


def attend(queries, keys, values, log_gates):
    row_count = queries.shape[0]
    head_count = log_gates.shape[1]
    head_width = queries.shape[1] // head_count
    score_scale = head_width ** (-0.5)
    first_row = lax.axis_index("sp") * row_count
    query_heads = queries.reshape(row_count, head_count, head_width)
    query_gates = log_gates.T
    query_positions = first_row + jnp.arange(row_count, dtype=jnp.int32)
    initial = (
        jnp.full((head_count, row_count), -1e30, jnp.float32),
        jnp.zeros((head_count, row_count), jnp.float32),
        jnp.zeros((head_count, row_count, head_width), jnp.float32),
    )
    carried = initial
    key_piece = lax.all_gather(keys.astype(jnp.float32), "sp", axis=0, tiled=True).astype(
        jnp.bfloat16
    )
    value_piece = lax.all_gather(values.astype(jnp.float32), "sp", axis=0, tiled=True).astype(
        jnp.bfloat16
    )
    gate_piece = lax.all_gather(log_gates, "sp", axis=0, tiled=True)
    length = key_piece.shape[0]
    block_rows = math.gcd(length, 2048)
    block_count = length // block_rows
    key_blocks = key_piece.reshape(block_count, block_rows, head_count, head_width)
    value_blocks = value_piece.reshape(block_count, block_rows, head_count, head_width)
    gate_blocks = gate_piece.reshape(block_count, block_rows, head_count)
    offsets = jnp.arange(block_count, dtype=jnp.int32) * block_rows

    def one_block(state, inputs):
        current_key_block, value_block, gate_block, offset = inputs

        def work(current):
            running_max, running_sum, accumulated = current
            scores = (
                jnp.einsum(
                    "qhd,khd->hqk",
                    query_heads,
                    current_key_block,
                    preferred_element_type=jnp.float32,
                )
                * score_scale
            )
            scores = scores + query_gates[:, :, None] - gate_block.T[:, None, :]
            key_positions = offset + jnp.arange(block_rows, dtype=jnp.int32)
            causal = (query_positions[:, None] >= key_positions[None, :])[None]
            scores = jnp.where(causal, scores, -1e30)
            new_max = jnp.maximum(running_max, jnp.max(scores, axis=-1))
            weights = jnp.where(causal, jnp.exp(scores - new_max[:, :, None]), 0.0)
            rescale = jnp.exp(running_max - new_max)
            running_sum = running_sum * rescale + jnp.sum(weights, axis=-1)
            product = jnp.einsum(
                "hqk,khd->hqd",
                weights.astype(jnp.bfloat16),
                value_block,
                preferred_element_type=jnp.float32,
            )
            accumulated = accumulated * rescale[:, :, None] + product
            return (new_max, running_sum, accumulated)

        state = lax.cond(offset <= first_row + row_count - 1, work, lambda current: current, state)
        return (state, None)

    carried, _ = lax.scan(one_block, carried, (key_blocks, value_blocks, gate_blocks, offsets))
    running_max, running_sum, accumulated = carried
    attended = accumulated / running_sum[:, :, None]
    return (
        attended.transpose(1, 0, 2).reshape(row_count, head_count * head_width).astype(jnp.bfloat16)
    )


def body(residual, queries, keys, values, log_gates, w_out, norm_gain, w_gate, w_up, w_down):
    attended = attend(queries, keys, values, log_gates)
    row_count = attended.shape[0]
    per_device = row_count // lax.axis_size("tp")
    my_first = lax.axis_index("tp") * per_device
    projected = lax.psum(
        jnp.dot(attended, w_out, preferred_element_type=jnp.float32).astype(jnp.bfloat16), "tp"
    ).astype(jnp.float32)
    mixed_all = (residual.astype(jnp.float32) + projected).astype(jnp.bfloat16)
    normed_all = normalize(mixed_all, norm_gain)
    mixed = lax.dynamic_slice_in_dim(mixed_all, my_first, per_device, 0)
    gate_whole = lax.all_gather(w_gate, "sp", axis=0, tiled=True)
    up_whole = lax.all_gather(w_up, "sp", axis=0, tiled=True)
    down_whole = lax.all_gather(w_down, "sp", axis=1, tiled=True)
    gate_proj = jnp.dot(normed_all, gate_whole, preferred_element_type=jnp.float32)
    up_proj = jnp.dot(normed_all, up_whole, preferred_element_type=jnp.float32)
    hidden = (jax.nn.silu(gate_proj) * up_proj).astype(jnp.bfloat16)
    down_sum = lax.psum_scatter(
        jnp.dot(hidden, down_whole, preferred_element_type=jnp.float32).astype(jnp.bfloat16),
        "tp",
        scatter_dimension=0,
        tiled=True,
    ).astype(jnp.float32)
    summed = mixed.astype(jnp.float32) + 0.5 * down_sum
    scaled = summed * lax.rsqrt(jnp.mean(summed * summed, axis=-1, keepdims=True) + 1e-06)
    return scaled.astype(jnp.bfloat16)


MESH = pl.DeviceIdType.MESH


def send(src, dst, sems, index, target):
    return pltpu.make_async_remote_copy(
        src_ref=src,
        dst_ref=dst,
        send_sem=sems.at[(0, *index)],
        recv_sem=sems.at[(1, *index)],
        device_id=target,
        device_id_type=MESH,
    )


def layer_kernel(
    n, tp, chunk,
    q_ref, k_ref, v_ref, g_ref, gt_ref, residual_ref, w_out_ref, gain_ref, wg_ref, wu_ref, wd_ref,
    out_ref,
    k_all, v_all, gt_all, att, proj, pc_buf, px_send, px_buf, mixed, normed,
    wg_all, wu_all, wd_all, hid, part, c_buf, x_send, x_buf, z_send, z_buf,
    kv_sems, w_sems, y_sems, pc_sems, px_sems, nz_sems, nx_sems, nc_sems, c_sems, x_sems, z_sems, o_sems,
):
    me = lax.axis_index("sp")
    t = lax.axis_index("tp")
    g = lax.axis_index("grp")
    x, c = t // 2, t % 2
    nx = tp // 2
    mate = x * 2 + (1 - c)
    rows = q_ref.shape[0]
    sub = rows // tp
    width = residual_ref.shape[1]
    heads = g_ref.shape[1]
    head = q_ref.shape[1] // heads
    depth = wg_ref.shape[0]
    ff = wg_ref.shape[1]
    half = depth // 2
    dcols = wd_ref.shape[1]
    dhalf = dcols // 2

    def there(d):
        return lax.rem(me + d, n)

    def origin(d):
        return lax.rem(me + n - d, n)

    def across(dx):
        return lax.rem(x + dx, nx)

    barrier = pltpu.get_barrier_semaphore()
    for d in range(1, n):
        pl.semaphore_signal(barrier, inc=1, device_id={"sp": there(d)}, device_id_type=MESH)
    for dx in range(1, nx):
        pl.semaphore_signal(
            barrier, inc=1, device_id={"tp": across(dx) * 2 + c}, device_id_type=MESH
        )
    pl.semaphore_signal(barrier, inc=1, device_id={"tp": mate}, device_id_type=MESH)
    pl.semaphore_signal(barrier, inc=1, device_id={"grp": 1 - g}, device_id_type=MESH)
    pl.semaphore_wait(barrier, n - 1 + nx - 1 + 2)

    def kv_copies(d):
        target = {"sp": lax.rem(me + 1, n)}
        own = (k_ref, v_ref, gt_ref)
        held = (k_all, v_all, gt_all)
        return [
            send(
                own[i] if d == 1 else held[i].at[d - 2], held[i].at[d - 1], kv_sems, (d - 1, i), target
            )
            for i in range(3)
        ]

    @pl.when(me + 1 < n)
    def _():
        for copy in kv_copies(1):
            copy.start()

    last = ff - (n - 1) * chunk
    my_rows = pl.ds(pl.multiple_of(g * half, half), half)
    my_cols = pl.ds(pl.multiple_of(g * dhalf, dhalf), dhalf)

    def w_copies(d, size):
        j = there(d)
        place = pl.ds(pl.multiple_of(jnp.minimum(j * chunk, ff - size), 128), size)
        target = {"sp": j}
        return (
            send(wg_ref.at[my_rows, place], wg_all.at[d, my_rows, :size], w_sems, (d - 1, 0), target),
            send(wu_ref.at[my_rows, place], wu_all.at[d, my_rows, :size], w_sems, (d - 1, 1), target),
            send(wd_ref.at[place, my_cols], wd_all.at[d, :size, my_cols], w_sems, (d - 1, 2), target),
        )

    def y_copies(d, size):
        target = {"grp": 1 - g}
        gate = wg_all.at[d, my_rows, :size]
        up = wu_all.at[d, my_rows, :size]
        down = wd_all.at[d, :size, my_cols]
        return (
            send(gate, gate, y_sems, (d - 1, 0), target),
            send(up, up, y_sems, (d - 1, 1), target),
            send(down, down, y_sems, (d - 1, 2), target),
        )

    def by_window(owner, work):
        pl.when(owner < n - 1)(lambda: work(chunk))
        pl.when(owner == n - 1)(lambda: work(last))

    def start_weights(d):
        def work(size):
            for copy in w_copies(d, size):
                copy.start()

        by_window(there(d), work)

    def pass_weights(d):
        def work(size):
            for copy, forward in zip(w_copies(d, size), y_copies(d, size)):
                copy.wait_recv()
                forward.start()

        by_window(me, work)

    for d in range(1, n):

        @pl.when(me + d >= n)
        def _(d=d):
            start_weights(d)

    def own_copies(size):
        mine = pl.ds(pl.multiple_of(jnp.minimum(me * chunk, ff - size), 128), size)
        return (
            pltpu.make_async_copy(wg_ref.at[:, mine], wg_all.at[0, :, :size], o_sems.at[0]),
            pltpu.make_async_copy(wu_ref.at[:, mine], wu_all.at[0, :, :size], o_sems.at[1]),
            pltpu.make_async_copy(wd_ref.at[mine, :], wd_all.at[0, :size, :], o_sems.at[2]),
        )

    def own_weights(size):
        for copy in own_copies(size):
            copy.start()
        if size < chunk:
            for d in range(n):
                wg_all[d, :, size:] = jnp.zeros((depth, chunk - size), jnp.bfloat16)
                wu_all[d, :, size:] = jnp.zeros((depth, chunk - size), jnp.bfloat16)
                wd_all[d, size:, :] = jnp.zeros((chunk - size, dcols), jnp.bfloat16)

    by_window(me, own_weights)

    for d in range(1, n):
        if d == n - 1:
            for e in range(1, n):

                @pl.when(me + e < n)
                def _(e=e):
                    start_weights(e)

        @pl.when(me >= d)
        def _(d=d):
            arrived = kv_copies(d)
            forwards = kv_copies(d + 1) if d + 1 < n else [None] * 3
            for copy, forward in zip(arrived, forwards):
                copy.wait_recv()
                if forward is not None:
                    pl.when(me + 1 < n)(forward.start)

        @pl.when(me < d)
        def _(d=d):
            k_all[d - 1] = jnp.zeros_like(k_ref)
            v_all[d - 1] = jnp.zeros_like(v_ref)
            gt_all[d - 1] = jnp.zeros_like(gt_ref)

    pair = 128 // head
    lane = lax.broadcasted_iota(jnp.int32, (rows, 128), 1)
    causal = lax.broadcasted_iota(jnp.int32, (rows, rows), 0) >= lax.broadcasted_iota(
        jnp.int32, (rows, rows), 1
    )
    contract = (((1,), (1,)), ((), ()))
    for p in range(heads // pair):
        cols = slice(p * 128, (p + 1) * 128)
        q_pair = q_ref[:, cols]
        joined = jnp.zeros((rows, 128), jnp.float32)
        for i in range(pair):
            h = p * pair + i
            inside = (lane >= i * head) & (lane < (i + 1) * head)
            q_head = jnp.where(inside, q_pair, jnp.zeros_like(q_pair))
            g_query = g_ref[:, h : h + 1]
            scores = []
            for d in range(n):
                k_pair = k_ref[:, cols] if d == 0 else k_all[d - 1, :, cols]
                g_key = gt_ref[h : h + 1, :] if d == 0 else gt_all[d - 1, h : h + 1, :]
                score = (
                    lax.dot_general(q_head, k_pair, contract, preferred_element_type=jnp.float32)
                    * head ** (-0.5)
                    + g_query
                    - g_key
                )
                allowed = causal if d == 0 else (jnp.zeros((rows, rows), jnp.int32) + me) >= d
                scores.append(jnp.where(allowed, score, -1e30))
            peak = functools.reduce(
                jnp.maximum, [jnp.max(score, axis=-1, keepdims=True) for score in scores]
            )
            total = jnp.zeros((rows, 1), jnp.float32)
            summed = jnp.zeros((rows, 128), jnp.float32)
            for d in range(n):
                v_pair = v_ref[:, cols] if d == 0 else v_all[d - 1, :, cols]
                weight = jnp.exp(scores[d] - peak)
                total += jnp.sum(weight, axis=-1, keepdims=True)
                summed += jnp.dot(
                    weight.astype(jnp.bfloat16), v_pair, preferred_element_type=jnp.float32
                )
            joined = jnp.where(inside, summed / total, joined)
        att[:, cols] = joined.astype(jnp.bfloat16)

    pass_weights(1)
    for k in range(width // 512):
        cols = slice(k * 512, (k + 1) * 512)
        proj[:, cols] = jnp.dot(
            att[...], w_out_ref[:, cols], preferred_element_type=jnp.float32
        ).astype(jnp.bfloat16)

    def block(index):
        return pl.ds(pl.multiple_of(index * sub, sub), sub)

    pc = [
        send(proj.at[block(across(dx) * 2 + 1 - c)], pc_buf.at[dx], pc_sems, (dx,), {"tp": mate})
        for dx in range(nx)
    ]
    for copy in pc:
        copy.start()
    px = [
        send(px_send.at[dx], px_buf.at[dx], px_sems, (dx,), {"tp": across(dx) * 2 + c})
        for dx in range(nx)
    ]
    for dx in range(1, nx):
        pc[dx].wait_recv()
        px_send[dx] = (
            proj[block(across(dx) * 2 + c), :].astype(jnp.float32) + pc_buf[dx].astype(jnp.float32)
        ).astype(jnp.bfloat16)
        px[dx].start()
    if n > 2:
        pass_weights(2)
    pc[0].wait_recv()
    acc = proj[block(t), :].astype(jnp.float32) + pc_buf[0].astype(jnp.float32)
    for dx in range(1, nx):
        px[dx].wait_recv()
        acc += px_buf[dx].astype(jnp.float32)
    mix = (residual_ref[block(t), :].astype(jnp.float32) + acc).astype(jnp.bfloat16)
    mixed[...] = mix
    floats = mix.astype(jnp.float32)
    scale = lax.rsqrt(jnp.mean(floats * floats, axis=-1, keepdims=True) + 1e-06)
    normed[me, block(t), :] = (floats * scale * gain_ref[...]).astype(jnp.bfloat16)

    own = normed.at[me, block(t)]
    nz = [send(own, own, nz_sems, (d,), {"sp": there(d)}) for d in range(n)]
    for d in range(1, n):
        nz[d].start()

    def spread(d):
        piece = normed.at[origin(d), block(t)]
        copies = [send(piece, piece, nc_sems, (d, 0), {"tp": mate})]
        for dx in range(1, nx):
            copies.append(send(piece, piece, nx_sems, (d, dx), {"tp": across(dx) * 2 + c}))
        return copies

    def relay(d, dx):
        piece = normed.at[origin(d), block(lax.rem(x + nx - dx, nx) * 2 + c)]
        return send(piece, piece, nc_sems, (d, dx), {"tp": mate})

    spreads = [spread(d) for d in range(n)]
    for copy in spreads[0]:
        copy.start()
    for d in range(3, n):
        pass_weights(d)

    def relay_all(d):
        for dx in range(1, nx):
            spreads[d][dx].wait_recv()
            relay(d, dx).start()

    relay_all(0)
    for d in range(1, n):
        nz[d].wait_recv()
        for copy in spreads[d]:
            copy.start()
        if d > 1:
            relay_all(d - 1)

    def y_arrived(size):
        for copy in own_copies(size):
            copy.wait()
        for d in range(1, n):
            for copy in y_copies(d, size):
                copy.wait_recv()

    by_window(me, y_arrived)

    def c_copy(d, dx):
        j = origin(d)
        return send(
            part.at[j, block(across(dx) * 2 + 1 - c)], c_buf.at[d, dx], c_sems, (d, dx), {"tp": mate}
        )

    def feed(d):
        j = origin(d)
        spreads[d][0].wait_recv()
        for dx in range(1, nx):
            relay(d, dx).wait_recv()
        gate = jnp.zeros((rows, chunk), jnp.float32)
        up = jnp.zeros((rows, chunk), jnp.float32)
        for e in range(n):
            piece = normed[j, :, pl.ds(pl.multiple_of(origin(e) * depth, depth), depth)]
            gate += jnp.dot(piece, wg_all[e], preferred_element_type=jnp.float32)
            up += jnp.dot(piece, wu_all[e], preferred_element_type=jnp.float32)
        hid[...] = (gate / (1.0 + jnp.exp(-gate)) * up).astype(jnp.bfloat16)
        for e in range(n):
            part[j, :, pl.ds(pl.multiple_of(origin(e) * dcols, dcols), dcols)] = jnp.dot(
                hid[...], wd_all[e], preferred_element_type=jnp.float32
            ).astype(jnp.bfloat16)
        for dx in range(nx):
            c_copy(d, dx).start()

    def x_copy(d, dx):
        return send(x_send.at[d, dx], x_buf.at[d, dx], x_sems, (d, dx), {"tp": across(dx) * 2 + c})

    def z_copy(d):
        return send(z_send.at[d], z_buf.at[d], z_sems, (d,), {"sp": origin(d)})

    def over_x(d):
        for dx in range(1, nx):
            c_copy(d, dx).wait_recv()
            x_send[d, dx] = (
                part[origin(d), block(across(dx) * 2 + c), :].astype(jnp.float32)
                + c_buf[d, dx].astype(jnp.float32)
            ).astype(jnp.bfloat16)
            x_copy(d, dx).start()

    def over_z(d):
        c_copy(d, 0).wait_recv()
        acc = part[origin(d), block(t), :].astype(jnp.float32) + c_buf[d, 0].astype(jnp.float32)
        for dx in range(1, nx):
            x_copy(d, dx).wait_recv()
            acc += x_buf[d, dx].astype(jnp.float32)
        if d != 0:
            z_send[d] = acc.astype(jnp.bfloat16)
            z_copy(d).start()
        return acc

    for d in range(n):
        if d == n - 1:
            relay_all(d)
        feed(d)
        if d > 0:
            over_x(d - 1)
        if d > 2:
            over_z(d - 2)
    over_x(n - 1)
    for d in range(max(1, n - 2), n):
        over_z(d)
    acc = over_z(0)
    for d in range(1, n):
        z_copy(d).wait_recv()
        acc += z_buf[d].astype(jnp.float32)
    summed = mixed[...].astype(jnp.float32) + 0.5 * acc
    scale = lax.rsqrt(jnp.mean(summed * summed, axis=-1, keepdims=True) + 1e-06)
    out_ref[...] = (summed * scale).astype(jnp.bfloat16)

    for copy in pc:
        copy.wait_send()
    for dx in range(1, nx):
        px[dx].wait_send()
    for d in range(n):
        for copy in spreads[d]:
            copy.wait_send()
        for dx in range(1, nx):
            relay(d, dx).wait_send()
            x_copy(d, dx).wait_send()
        for dx in range(nx):
            c_copy(d, dx).wait_send()
    for d in range(1, n):
        nz[d].wait_send()
        z_copy(d).wait_send()

        def w_sent(size, d=d):
            for copy in w_copies(d, size):
                copy.wait_send()

        def y_sent(size, d=d):
            for copy in y_copies(d, size):
                copy.wait_send()

        by_window(there(d), w_sent)
        by_window(me, y_sent)

        @pl.when((me >= d - 1) & (me + 1 < n))
        def _(d=d):
            for copy in kv_copies(d):
                copy.wait_send()


def fused_body(residual, queries, keys, values, log_gates, w_out, norm_gain, w_gate, w_up, w_down):
    n, tp = lax.axis_size("sp"), lax.axis_size("tp")
    rows, width = residual.shape
    sub = rows // tp
    nx = tp // 2
    heads = log_gates.shape[1]
    depth, ff = w_gate.shape
    dcols = w_down.shape[1]
    chunk = window(ff, n)
    gates_t = jnp.pad(log_gates.T, ((0, -heads % 8), (0, 0)))
    bf16, f32 = jnp.bfloat16, jnp.float32
    shapes = [
        ((n - 1, *keys.shape), bf16),
        ((n - 1, *values.shape), bf16),
        ((n - 1, *gates_t.shape), f32),
        (queries.shape, bf16),
        ((rows, width), bf16),
        ((nx, sub, width), bf16),
        ((nx, sub, width), bf16),
        ((nx, sub, width), bf16),
        ((sub, width), bf16),
        ((n, rows, width), bf16),
        ((n, depth, chunk), bf16),
        ((n, depth, chunk), bf16),
        ((n, chunk, dcols), bf16),
        ((rows, chunk), bf16),
        ((n, rows, width), bf16),
        ((n, nx, sub, width), bf16),
        ((n, nx, sub, width), bf16),
        ((n, nx, sub, width), bf16),
        ((n, sub, width), bf16),
        ((n, sub, width), bf16),
    ]
    sems = [
        (2, n - 1, 3),
        (2, n - 1, 3),
        (2, n - 1, 3),
        (2, nx),
        (2, nx),
        (2, n),
        (2, n, nx),
        (2, n, nx),
        (2, n, nx),
        (2, n, nx),
        (2, n),
        (3,),
    ]
    return pl.pallas_call(
        functools.partial(layer_kernel, n, tp, chunk),
        out_shape=jax.ShapeDtypeStruct((sub, width), bf16),
        in_specs=[pl.BlockSpec(memory_space=pltpu.VMEM)] * 8
        + [pl.BlockSpec(memory_space=pl.ANY)] * 3,
        out_specs=pl.BlockSpec(memory_space=pltpu.VMEM),
        scratch_shapes=[pltpu.VMEM(shape, dtype) for shape, dtype in shapes]
        + [pltpu.SemaphoreType.DMA(shape) for shape in sems],
        compiler_params=pltpu.CompilerParams(
            collective_id=0, has_side_effects=True, vmem_limit_bytes=60 * 1024 * 1024
        ),
    )(
        queries, keys, values, log_gates, gates_t, residual, w_out, norm_gain[None, :],
        w_gate, w_up, w_down,
    )


def window(ff, n):
    return -(-ff // (n * 128)) * 128


def fits(mesh, shapes):
    residual, queries, gates, gate = shapes
    n, tp, grp = mesh.shape["sp"], mesh.shape["tp"], mesh.shape["grp"]
    ff = gate[1] // tp
    heads = gates[1] // tp
    head = queries[1] // gates[1]
    rows = residual[0] // (grp * n)
    return (
        grp == 2
        and 2 <= n <= 4
        and tp % 2 == 0
        and ff % 128 == 0
        and window(ff, n) * (n - 1) < ff
        and 128 % head == 0
        and (heads * head) % 128 == 0
        and rows % (16 * tp) == 0
        and rows * n * residual[1] <= 1 << 21
    )


def solution(mesh):
    in_specs = (
        P(("grp", "sp"), None),
        P(("grp", "sp"), "tp"),
        P(("grp", "sp"), "tp"),
        P(("grp", "sp"), "tp"),
        P(("grp", "sp"), "tp"),
        P("tp", None),
        P(),
        P("sp", "tp"),
        P("sp", "tp"),
        P("tp", "sp"),
    )
    out_specs = P(("grp", "sp", "tp"), None)

    def layer(*args):
        residual, queries, _, _, log_gates, _, _, w_gate, _, _ = args
        shapes = (residual.shape, queries.shape, log_gates.shape, w_gate.shape)
        chosen = fused_body if fits(mesh, shapes) else body
        return jax.shard_map(
            chosen, mesh=mesh, in_specs=in_specs, out_specs=out_specs, check_vma=False
        )(*args)

    return layer
```
